32 devices in a mesh: sp: 16 (over z, x, core), tp: 2 (over y).
Axes of the slice: x: 2, y: 2, z: 4, core: 2. Of those that a mesh axis runs over, the one named last changes fastest.
Arguments:
- queries: bfloat16 [10240, 1024], P('sp', 'tp'), may hold values from -160 to 160
- keys: bfloat16 [10240, 256], P('sp', 'tp'), may hold values from -24 to 24
- values: bfloat16 [10240, 256], P('sp', 'tp'), may hold values from -6 to 6
- documents: int32 [10240], P('sp'), may hold values from 0 to 3, never falling along the last dimension, each value on 1 to 5120 neighbouring positions
- sinks: float32 [16], P('tp'), may hold values from -1 to 4
- out_weight: bfloat16 [1024, 2048], replicated, may hold values from -0.1875 to 0.1875
- residual: bfloat16 [10240, 2048], P(('sp', 'tp')), may hold values from -3 to 3
- norm_gain: float32 [2048], replicated, may hold values from 0.1 to 1.9
- up_weight: bfloat16 [2048, 8192], P('sp', 'tp'), may hold values from -0.125 to 0.125
- down_weight: bfloat16 [8192, 2048], P('tp', 'sp'), may hold values from -0.0625 to 0.0625
Outputs:
- layer_out: bfloat16 [10240, 2048], P(('sp', 'tp'))
The draws below stay inside these ranges and needn't reach their ends.
Inputs may be any that keep to these rules, and one draw needn't show every extreme that they name: `documents`: document numbers never fall along the positions; each document holds at most 5120 positions.
All inputs are finite; a program needn't handle non-finite values.
Results may differ from the reference program's by a relative error of at most 0.0095.
Values may be sent and summed in bfloat16 or wider, within the bound.
A program may use at most 128 MiB of HBM per device.

```python
import math
import jax
import jax.numpy as jnp
import numpy as np
from jax import lax

D = 2048
QUERY_HEADS = 16
KEY_VALUE_HEADS = 4
HEAD_SIZE = 64
FF = 8192
WINDOW_REACH = 128
TOK_DEV = 640
PACK_TOKENS = 10240
ATTN = 1024
FF_DEV = 4096
DOCS = 4
N_SP = 16
N_TP = 2


def drawn(key):
    starting_keys = jax.random.normal(jax.random.fold_in(key, 11), (PACK_TOKENS, KEY_VALUE_HEADS, HEAD_SIZE), jnp.float32)
    base_queries = jax.random.normal(jax.random.fold_in(key, 12), (PACK_TOKENS, QUERY_HEADS, HEAD_SIZE), jnp.float32)
    output_keys = starting_keys
    output_queries = base_queries
    return (output_queries.reshape(PACK_TOKENS, QUERY_HEADS * HEAD_SIZE).astype(jnp.bfloat16), output_keys.reshape(PACK_TOKENS, KEY_VALUE_HEADS * HEAD_SIZE).astype(jnp.bfloat16))


def draw_queries(key, part):
    return drawn(key)[0]


def draw_keys(key, part):
    return drawn(key)[1]


def shard_levels(stream_key, dims, cuts, low, largest):
    level = 1.0
    for dim, blocks in cuts:
        heights = jax.random.uniform(jax.random.fold_in(jax.random.fold_in(stream_key, 6), dim), (blocks,), jnp.float32, low / len(cuts), largest / len(cuts))
        level = level * jnp.repeat(jnp.exp(heights), dims[dim] // blocks).reshape((-1,) + (1,) * (len(dims) - 1 - dim))
    return level


def split_up(count, total, limit, lean):
    loads = [(1 << 20) // math.isqrt(grade ** lean) + 1 for grade in range(2, count + 1)]
    surplus, counts = total - limit - (count - 1), [1] * (count - 1)
    while surplus > 0:
        free = [i for i in range(count - 1) if counts[i] < limit]
        mass, budget = sum([loads[i] for i in free]), surplus
        for i in free:
            more = min(limit - counts[i], max(1, budget * loads[i] // mass), surplus)
            counts[i] = counts[i] + more
            surplus = surplus - more
    return np.array([limit] + counts)


def ragged(rng, amount, total, limit, lean):
    if amount == 2:
        one = jax.random.randint(rng, (), max(1, total - limit), min(limit, total - 1) + 1)
        return jnp.stack([one, total - one])
    lengths = jnp.asarray(split_up(amount, total, limit, lean), jnp.int32)
    couples = (amount - 1) // 2
    giver, taker = lengths[1:1 + 2 * couples:2], lengths[2:2 + 2 * couples:2]
    margin = jnp.minimum(giver - 1, limit - taker)
    shifted = jax.random.randint(jax.random.fold_in(rng, 1), (couples,), 0, 1 << 20) % (margin + 1)
    lengths = lengths.at[1:1 + 2 * couples:2].set(giver - shifted).at[2:2 + 2 * couples:2].set(taker + shifted)
    return lengths[jax.random.permutation(jax.random.fold_in(rng, 2), amount)]


def noise(own_key, shape, spread, bound, pieces=(), kind=jnp.bfloat16):
    array = jax.random.normal(own_key, shape, jnp.float32) * spread
    if len(pieces) > 0:
        array = shard_levels(own_key, shape, pieces, -0.22, 0.18) * array
    return jnp.clip(array, min=-bound, max=bound).astype(kind)


def setup_inputs(seed: int = 0) -> dict:
    streams_of = jax.random.split(jax.random.key(seed), 11)
    queries = draw_queries(jax.random.fold_in(streams_of[10], 71), 0)
    keys = draw_keys(jax.random.fold_in(streams_of[10], 71), 0)
    values = noise(streams_of[2], (PACK_TOKENS, KEY_VALUE_HEADS * HEAD_SIZE), 1.0, 6.0, ((0, 16), (1, 2)))
    documents = jnp.searchsorted(jnp.cumsum(ragged(streams_of[3], DOCS, PACK_TOKENS, 8 * TOK_DEV, 1)), jnp.arange(PACK_TOKENS), side="right").astype(jnp.int32)
    sinks = jnp.clip(-1.0 + 5.0 * jax.random.uniform(streams_of[4], (QUERY_HEADS,), jnp.float32) ** shard_levels(streams_of[4], (QUERY_HEADS,), ((0, 2),), -0.2, 0.2), -1.0, 4.0)
    out_weight = noise(streams_of[5], (ATTN, D), ATTN ** -0.5, 0.1875)
    residual = noise(streams_of[6], (PACK_TOKENS, D), 0.5, 3.0, ((0, 32),))
    norm_gain = jnp.clip(1.0 + 0.18 * jax.random.normal(streams_of[7], (D,), jnp.float32), 0.1, 1.9)
    up_weight = noise(streams_of[8], (D, FF), D ** -0.5, 0.125, ((0, 16), (1, 2)))
    down_weight = noise(streams_of[9], (FF, D), FF ** -0.5, 0.0625, ((0, 2), (1, 16)))
    return {"queries": queries, "keys": keys, "values": values, "documents": documents, "sinks": sinks, "out_weight": out_weight, "residual": residual, "norm_gain": norm_gain, "up_weight": up_weight, "down_weight": down_weight}


masked_score = -1e+30
epsilon = 1e-06

def rounded(value):
    return lax.optimization_barrier(value.astype(jnp.bfloat16))

def reference(queries, keys, values, documents, sinks, out_weight, residual, norm_gain, up_weight, down_weight):
    query_group = QUERY_HEADS // KEY_VALUE_HEADS
    block_list = PACK_TOKENS // WINDOW_REACH
    key_matrix = jnp.concatenate([jnp.zeros((WINDOW_REACH, KEY_VALUE_HEADS * HEAD_SIZE), jnp.bfloat16), keys], axis=0).reshape(block_list + 1, WINDOW_REACH, KEY_VALUE_HEADS, HEAD_SIZE)
    value_matrix = jnp.concatenate([jnp.zeros((WINDOW_REACH, KEY_VALUE_HEADS * HEAD_SIZE), jnp.bfloat16), values], axis=0).reshape(block_list + 1, WINDOW_REACH, KEY_VALUE_HEADS, HEAD_SIZE)
    doc_ids = documents.astype(jnp.int32)
    key_docs = jnp.concatenate([jnp.full((WINDOW_REACH,), -1, jnp.int32), doc_ids], axis=0).reshape(block_list + 1, WINDOW_REACH)
    query_docs = doc_ids.reshape(block_list, WINDOW_REACH)
    grouped_queries = queries.reshape(block_list, WINDOW_REACH, KEY_VALUE_HEADS, query_group, HEAD_SIZE)
    head_sink_logit = sinks.astype(jnp.float32).reshape(KEY_VALUE_HEADS, query_group, 1)
    row_index = jnp.arange(WINDOW_REACH, dtype=jnp.int32)[:, None]
    col_index = jnp.arange(2 * WINDOW_REACH, dtype=jnp.int32)[None, :]
    distance = WINDOW_REACH + row_index - col_index
    near = (distance >= 0) & (distance < WINDOW_REACH)

    def one_block(items):
        block_queries, early_keys, late_keys, early_values, late_values, early_docs, late_docs, own_docs = items
        band_keys = jnp.concatenate([early_keys, late_keys], axis=0).astype(jnp.float32)
        band_values = jnp.concatenate([early_values, late_values], axis=0).astype(jnp.float32)
        band_docs = jnp.concatenate([early_docs, late_docs], axis=0)
        visible = (near & (band_docs[None, :] == own_docs[:, None]))[None, None]
        scores = jnp.einsum('qhgd,shd->hgqs', block_queries.astype(jnp.float32), band_keys) * HEAD_SIZE ** (-0.5)
        scores = jnp.where(visible, scores, masked_score)
        top = jnp.maximum(lax.optimization_barrier(jnp.max(scores, axis=-1)), head_sink_logit)
        exponent = jnp.where(visible, jnp.exp(scores - top[..., None]), 0.0)
        total = jnp.exp(head_sink_logit - top) + lax.optimization_barrier(jnp.sum(exponent, axis=-1))
        shares = rounded(exponent / total[..., None])
        attended = jnp.einsum('hgqs,shd->qhgd', shares.astype(jnp.float32), band_values)
        return attended.astype(jnp.bfloat16).reshape(WINDOW_REACH, QUERY_HEADS * HEAD_SIZE)
    attended = lax.map(one_block, (grouped_queries, key_matrix[:-1], key_matrix[1:], value_matrix[:-1], value_matrix[1:], key_docs[:-1], key_docs[1:], query_docs))
    attended = attended.reshape(PACK_TOKENS, QUERY_HEADS * HEAD_SIZE)
    projected = jnp.dot(attended.astype(jnp.float32), out_weight.astype(jnp.float32), preferred_element_type=jnp.float32)
    mixed = rounded(residual.astype(jnp.float32) + rounded(projected).astype(jnp.float32))
    widened = mixed.astype(jnp.float32)
    normed = (widened * lax.rsqrt(lax.optimization_barrier(jnp.mean(widened * widened, axis=-1, keepdims=True)) + epsilon) * norm_gain.astype(jnp.float32)).astype(jnp.bfloat16)
    down_groups = down_weight.astype(jnp.float32).reshape(N_TP, FF_DEV, D)

    def mixer_block(rows):
        before = jnp.dot(rows.astype(jnp.float32), up_weight.astype(jnp.float32), preferred_element_type=jnp.float32)
        hidden = jnp.square(jax.nn.relu(before)).astype(jnp.bfloat16)
        parts = jnp.einsum('rnf,nfd->nrd', hidden.reshape(rows.shape[0], N_TP, FF_DEV).astype(jnp.float32), down_groups)
        return lax.optimization_barrier(jnp.sum(rounded(parts).astype(jnp.float32), axis=0))
    branch = lax.map(mixer_block, normed.reshape(N_SP, TOK_DEV, D)).reshape(PACK_TOKENS, D)
    return (widened + rounded(branch).astype(jnp.float32)).astype(jnp.bfloat16)
```

```python
import jax
import jax.numpy as jnp
from jax import lax
from jax.sharding import PartitionSpec as P

HEAD_SIZE = 64
WINDOW_REACH = 128


masked_score = -1e30
epsilon = 1e-06


def passed_along(shard, axis, by):
    peers = lax.axis_size(axis)
    pairs = [(i, i + by) for i in range(peers) if 0 <= i + by < peers]
    return lax.ppermute(shard, axis, pairs)


def rounded(value):
    return lax.optimization_barrier(value.astype(jnp.bfloat16))


def squared_relu(before):
    return jnp.square(jax.nn.relu(before)).astype(jnp.bfloat16)


def windowed_attention(queries, keys, values, documents, sinks):
    length = queries.shape[0]
    heads = queries.shape[1] // HEAD_SIZE
    kv_heads = keys.shape[1] // HEAD_SIZE
    query_group = heads // kv_heads
    block_list = length // WINDOW_REACH
    prev_keys, prev_values, prev_docs = passed_along(
        (
            keys[length - WINDOW_REACH :],
            values[length - WINDOW_REACH :],
            documents[length - WINDOW_REACH :],
        ),
        "sp",
        1,
    )
    offset = lax.axis_index("sp") * length
    key_matrix = jnp.concatenate([prev_keys, keys], axis=0).reshape(
        block_list + 1, WINDOW_REACH, kv_heads, HEAD_SIZE
    )
    value_matrix = jnp.concatenate([prev_values, values], axis=0).reshape(
        block_list + 1, WINDOW_REACH, kv_heads, HEAD_SIZE
    )
    key_docs = jnp.concatenate([prev_docs, documents], axis=0).reshape(block_list + 1, WINDOW_REACH)
    key_place = (
        offset - WINDOW_REACH + jnp.arange((block_list + 1) * WINDOW_REACH, dtype=jnp.int32)
    ).reshape(block_list + 1, WINDOW_REACH)
    band_keys = jnp.concatenate([key_matrix[:-1], key_matrix[1:]], axis=1)
    band_values = jnp.concatenate([value_matrix[:-1], value_matrix[1:]], axis=1)
    band_docs = jnp.concatenate([key_docs[:-1], key_docs[1:]], axis=1)
    band_place = jnp.concatenate([key_place[:-1], key_place[1:]], axis=1)
    query_docs = documents.reshape(block_list, WINDOW_REACH)
    grouped_queries = queries.reshape(block_list, WINDOW_REACH, kv_heads, query_group, HEAD_SIZE)
    scores = jnp.einsum(
        "nqhgd,nshd->nhgqs", grouped_queries, band_keys, preferred_element_type=jnp.float32
    ) * HEAD_SIZE ** (-0.5)
    row_index = jnp.arange(WINDOW_REACH, dtype=jnp.int32)[:, None]
    col_index = jnp.arange(2 * WINDOW_REACH, dtype=jnp.int32)[None, :]
    distance = WINDOW_REACH + row_index - col_index
    near = (distance >= 0) & (distance < WINDOW_REACH)
    visible = (
        near[None]
        & (band_docs[:, None, :] == query_docs[:, :, None])
        & (band_place[:, None, :] >= 0)
    )
    visible = visible[:, None, None]
    head_sink_logit = sinks.reshape(kv_heads, query_group)[None, :, :, None]
    scores = jnp.where(visible, scores, masked_score)
    top = jnp.maximum(jnp.max(scores, axis=-1), head_sink_logit)
    exponent = jnp.where(visible, jnp.exp(scores - top[..., None]), 0.0)
    total = jnp.exp(head_sink_logit - top) + jnp.sum(exponent, axis=-1)
    shares = (exponent / total[..., None]).astype(jnp.bfloat16)
    attended = jnp.einsum(
        "nhgqs,nshd->nqhgd", shares, band_values, preferred_element_type=jnp.float32
    )
    return attended.astype(jnp.bfloat16).reshape(length, heads * HEAD_SIZE)


def rotated(shard, axis, by):
    peers = lax.axis_size(axis)
    return lax.ppermute(shard, axis, [(i, (i + by) % peers) for i in range(peers)])


def row_block(array, index, rows):
    return lax.dynamic_slice_in_dim(array, index * rows, rows, axis=0)


def body(
    queries, keys, values, documents, sinks, out_weight, residual, norm_gain, up_weight, down_weight
):
    up_whole, down_whole = (
        lax.all_gather(up_weight, "sp", axis=0, tiled=True),
        lax.all_gather(down_weight, "sp", axis=1, tiled=True),
    )
    n_tp = lax.axis_size("tp")
    me = lax.axis_index("tp")
    rows = residual.shape[0]
    attended = windowed_attention(queries, keys, values, documents, sinks)
    width = attended.shape[1]
    token_heads = jnp.zeros((rows, width * n_tp), jnp.bfloat16)
    for by in range(n_tp):
        piece = row_block(attended, (me + by) % n_tp, rows)
        if by:
            piece = rotated(piece, "tp", by)
        token_heads = lax.dynamic_update_slice_in_dim(
            token_heads, piece, ((me - by) % n_tp) * width, axis=1
        )
    projected = jnp.dot(token_heads, out_weight, preferred_element_type=jnp.float32)
    mixed = rounded(residual.astype(jnp.float32) + rounded(projected).astype(jnp.float32))
    widened = mixed.astype(jnp.float32)
    normed = (
        widened
        * lax.rsqrt(jnp.mean(widened * widened, axis=-1, keepdims=True) + epsilon)
        * norm_gain
    ).astype(jnp.bfloat16)
    branch = 0.0
    for by in range(n_tp - 1, -1, -1):
        rows_in = rotated(normed, "tp", by) if by else normed
        hidden = squared_relu(jnp.dot(rows_in, up_whole, preferred_element_type=jnp.float32))
        partial = jnp.dot(hidden, down_whole, preferred_element_type=jnp.float32).astype(
            jnp.bfloat16
        )
        if by:
            partial = rotated(partial, "tp", n_tp - by)
        branch = branch + partial.astype(jnp.float32)
    return (widened + rounded(branch).astype(jnp.float32)).astype(jnp.bfloat16)


def solution(mesh):
    in_specs = (
        P("sp", "tp"),
        P("sp", "tp"),
        P("sp", "tp"),
        P("sp"),
        P("tp"),
        P(),
        P(("sp", "tp"), None),
        P(),
        P("sp", "tp"),
        P("tp", "sp"),
    )
    out_specs = P(("sp", "tp"), None)
    return jax.shard_map(body, mesh=mesh, in_specs=in_specs, out_specs=out_specs, check_vma=False)
```

```python
import jax
import jax.numpy as jnp
from jax import lax
from jax.sharding import PartitionSpec as P

HEAD_SIZE = 64
WINDOW_REACH = 128


masked_score = -1e30
epsilon = 1e-06


def passed_along(shard, axis, by):
    peers = lax.axis_size(axis)
    pairs = [(i, i + by) for i in range(peers) if 0 <= i + by < peers]
    return lax.ppermute(shard, axis, pairs)


def rounded(value):
    return lax.optimization_barrier(value.astype(jnp.bfloat16))


def squared_relu(before):
    return jnp.square(jax.nn.relu(before)).astype(jnp.bfloat16)


def windowed_attention(queries, keys, values, documents, sinks):
    length = queries.shape[0]
    heads = queries.shape[1] // HEAD_SIZE
    kv_heads = keys.shape[1] // HEAD_SIZE
    query_group = heads // kv_heads
    block_list = length // WINDOW_REACH
    prev_keys, prev_values, prev_docs = passed_along(
        (
            keys[length - WINDOW_REACH :],
            values[length - WINDOW_REACH :],
            documents[length - WINDOW_REACH :],
        ),
        "sp",
        1,
    )
    offset = lax.axis_index("sp") * length
    key_matrix = jnp.concatenate([prev_keys, keys], axis=0).reshape(
        block_list + 1, WINDOW_REACH, kv_heads, HEAD_SIZE
    )
    value_matrix = jnp.concatenate([prev_values, values], axis=0).reshape(
        block_list + 1, WINDOW_REACH, kv_heads, HEAD_SIZE
    )
    key_docs = jnp.concatenate([prev_docs, documents], axis=0).reshape(block_list + 1, WINDOW_REACH)
    key_place = (
        offset - WINDOW_REACH + jnp.arange((block_list + 1) * WINDOW_REACH, dtype=jnp.int32)
    ).reshape(block_list + 1, WINDOW_REACH)
    band_keys = jnp.concatenate([key_matrix[:-1], key_matrix[1:]], axis=1)
    band_values = jnp.concatenate([value_matrix[:-1], value_matrix[1:]], axis=1)
    band_docs = jnp.concatenate([key_docs[:-1], key_docs[1:]], axis=1)
    band_place = jnp.concatenate([key_place[:-1], key_place[1:]], axis=1)
    query_docs = documents.reshape(block_list, WINDOW_REACH)
    grouped_queries = queries.reshape(block_list, WINDOW_REACH, kv_heads, query_group, HEAD_SIZE)
    scores = jnp.einsum(
        "nqhgd,nshd->nhgqs", grouped_queries, band_keys, preferred_element_type=jnp.float32
    ) * HEAD_SIZE ** (-0.5)
    row_index = jnp.arange(WINDOW_REACH, dtype=jnp.int32)[:, None]
    col_index = jnp.arange(2 * WINDOW_REACH, dtype=jnp.int32)[None, :]
    distance = WINDOW_REACH + row_index - col_index
    near = (distance >= 0) & (distance < WINDOW_REACH)
    visible = (
        near[None]
        & (band_docs[:, None, :] == query_docs[:, :, None])
        & (band_place[:, None, :] >= 0)
    )
    visible = visible[:, None, None]
    head_sink_logit = sinks.reshape(kv_heads, query_group)[None, :, :, None]
    scores = jnp.where(visible, scores, masked_score)
    top = jnp.maximum(jnp.max(scores, axis=-1), head_sink_logit)
    exponent = jnp.where(visible, jnp.exp(scores - top[..., None]), 0.0)
    total = jnp.exp(head_sink_logit - top) + jnp.sum(exponent, axis=-1)
    shares = (exponent / total[..., None]).astype(jnp.bfloat16)
    attended = jnp.einsum(
        "nhgqs,nshd->nqhgd", shares, band_values, preferred_element_type=jnp.float32
    )
    return attended.astype(jnp.bfloat16).reshape(length, heads * HEAD_SIZE)


def rotated(shard, axis, by):
    peers = lax.axis_size(axis)
    return lax.ppermute(shard, axis, [(i, (i + by) % peers) for i in range(peers)])


def row_block(array, index, rows):
    return lax.dynamic_slice_in_dim(array, index * rows, rows, axis=0)


CORES = 2


def gathered_parity(shard, axis):
    peers = lax.axis_size("sp")
    groups = [list(range(core, peers, CORES)) for core in range(CORES)]
    return lax.all_gather(shard, "sp", axis=axis, tiled=True, axis_index_groups=groups)


def from_neighbour(array):
    peers = lax.axis_size("sp")
    return lax.ppermute(array, "sp", [(i, i ^ 1) for i in range(peers)])


def body(
    queries, keys, values, documents, sinks, out_weight, residual, norm_gain, up_weight, down_weight
):
    up_mine = gathered_parity(up_weight, 0)
    down_mine = gathered_parity(down_weight, 1)
    n_tp = lax.axis_size("tp")
    me = lax.axis_index("tp")
    first = lax.axis_index("sp") % CORES == 0
    rows, d_model = residual.shape
    attended = windowed_attention(queries, keys, values, documents, sinks)
    width = attended.shape[1]
    token_heads = jnp.zeros((rows, width * n_tp), jnp.bfloat16)
    for by in range(n_tp):
        piece = row_block(attended, (me + by) % n_tp, rows)
        if by:
            piece = rotated(piece, "tp", by)
        token_heads = lax.dynamic_update_slice_in_dim(
            token_heads, piece, ((me - by) % n_tp) * width, axis=1
        )
    projected = jnp.dot(token_heads, out_weight, preferred_element_type=jnp.float32)
    mixed = rounded(residual.astype(jnp.float32) + rounded(projected).astype(jnp.float32))
    widened = mixed.astype(jnp.float32)
    normed = (
        widened
        * lax.rsqrt(jnp.mean(widened * widened, axis=-1, keepdims=True) + epsilon)
        * norm_gain
    ).astype(jnp.bfloat16)
    split = normed.reshape(rows, -1, CORES, up_weight.shape[0])
    even, odd = (split[:, :, core].reshape(rows, -1) for core in range(CORES))
    halves = lax.optimization_barrier((jnp.where(first, even, odd), jnp.where(first, odd, even)))
    normed_mine, normed_theirs = (
        jnp.concatenate(
            [rotated(half, "tp", by) if by else half for by in range(n_tp - 1, -1, -1)], axis=0
        )
        for half in halves
    )
    up_theirs = from_neighbour(up_mine)
    before = jnp.dot(normed_mine, up_mine, preferred_element_type=jnp.float32)
    before = before + jnp.dot(normed_theirs, up_theirs, preferred_element_type=jnp.float32)
    hidden = lax.optimization_barrier(squared_relu(before))
    branches = []
    for weight in (down_mine, from_neighbour(down_mine)):
        branch = 0.0
        for place, by in enumerate(range(n_tp - 1, -1, -1)):
            partial = jnp.dot(
                hidden[place * rows : (place + 1) * rows],
                weight,
                preferred_element_type=jnp.float32,
            ).astype(jnp.bfloat16)
            if by:
                partial = rotated(partial, "tp", n_tp - by)
            branch = branch + partial.astype(jnp.float32)
        branches.append(branch.astype(jnp.bfloat16).reshape(rows, -1, down_weight.shape[1]))
    mine, theirs = branches
    branch = jnp.stack(
        [jnp.where(first, mine, theirs), jnp.where(first, theirs, mine)], axis=2
    ).reshape(rows, d_model)
    return (widened + rounded(branch).astype(jnp.float32)).astype(jnp.bfloat16)


def solution(mesh):
    in_specs = (
        P("sp", "tp"),
        P("sp", "tp"),
        P("sp", "tp"),
        P("sp"),
        P("tp"),
        P(),
        P(("sp", "tp"), None),
        P(),
        P("sp", "tp"),
        P("tp", "sp"),
    )
    out_specs = P(("sp", "tp"), None)
    return jax.shard_map(body, mesh=mesh, in_specs=in_specs, out_specs=out_specs, check_vma=False)
```
